32 devices in a mesh: grp: 2 (over y), sp: 4 (over z), tp: 4 (over x, core).
Axes of the slice: x: 2, y: 2, z: 4, core: 2. Of those that a mesh axis runs over, the one named last changes fastest.
Arguments:
- tokens: bfloat16 [2048, 2048], P(('grp', 'sp'), 'tp'), parts along dimension 0, may hold values from -6 to 6
- norm_gain: float32 [2048], replicated, may hold values from 0.1 to 1.9
- ret_query_weight: bfloat16 [2048, 256], P('sp', 'tp'), may hold values from -0.125 to 0.125
- ret_key_weight: bfloat16 [2048, 256], P('sp', 'tp'), may hold values from -0.125 to 0.125
- ret_value_weight: bfloat16 [2048, 512], P('sp', 'tp'), may hold values from -0.125 to 0.125
- fox_query_weight: bfloat16 [2048, 512], P('sp', 'tp'), may hold values from -8 to 8
- fox_key_weight: bfloat16 [2048, 512], P('sp', 'tp'), may hold values from -0.125 to 0.125
- fox_value_weight: bfloat16 [2048, 512], P('sp', 'tp'), may hold values from -0.125 to 0.125
- ret_decay: float32 [8], P('tp'), may hold values from -1 to 0, as said below
- ret_state: float32 [16, 32, 64], P(('grp', 'tp')), parts along dimension 0, may hold values from -64 to 64
- head_norm_gain: float32 [512], P('tp'), may hold values from 0.1 to 1.9
- fox_gates: float32 [2048, 8], P('grp', 'tp'), parts along dimension 0, may hold values from -3072 to 0, as said below
- ret_out_weight: bfloat16 [512, 2048], P('tp', 'sp'), may hold values from -0.1875 to 0.1875
- fox_out_weight: bfloat16 [512, 2048], P('tp', 'sp'), may hold values from -1 to 1
Outputs:
- mixed: bfloat16 [2048, 2048], P(('grp', 'sp', 'tp')), parts along dimension 0
The draws below stay inside these ranges and needn't reach their ends.
There are 2 independent parts, one for each index of `grp`. The reference program is written for one: setup_inputs(seed, part) draws one part's arguments, and reference() takes and returns one part's arrays. A program takes and returns all parts, laid end to end along the dimension named above; an argument that names none is the same for every part. Nothing has to cross between parts.
Inputs may be any that keep to these rules, and one draw needn't show every extreme that they name: `ret_decay`: each head's log decay is negative. `fox_gates`: along the positions each head's column never rises.
All inputs are finite; a program needn't handle non-finite values.
Results may differ from the reference program's by a relative error of at most 0.015.
The reference program's roundings to bfloat16 on the way count: a program that leaves them out, or rounds other values in their place, can miss the bound.
Values may be sent and summed in bfloat16 or wider, within the bound.
A program may use at most 64 MiB of HBM per device.

```python
import jax
import jax.numpy as jnp
from jax import lax

D = 2048
RETAIN_HEADS = 8
DK = 32
RETAIN_VALUE_DIM = 64
FH = 8
FD = 64
TOK_DEV = 256
TOKENS = 1024
N_TP = 4


def draw_fox_query_weight(key, part):
    keys = jax.random.split(jax.random.fold_in(key, 11), 1)
    columns = FH * FD
    return (jnp.clip(jax.random.normal(keys[0], (D, columns), jnp.float32), -6.0, 6.0) * D ** (-0.5)).astype(jnp.bfloat16)


def draw_ret_decay(key, part):
    keys = jax.random.split(jax.random.fold_in(key, 23), 3)
    order = jax.random.permutation(keys[0], RETAIN_HEADS)
    quick = order < RETAIN_HEADS // 2
    quick_rate = -1.0 / jax.random.uniform(keys[1], (RETAIN_HEADS,), jnp.float32, 30.0, 100.0)
    slow_rate = -jax.random.uniform(keys[2], (RETAIN_HEADS,), jnp.float32, 0.3, 2.0) / TOKENS
    return jnp.where(quick, quick_rate, slow_rate)


def draw_ret_state(key, part):
    source = jax.random.fold_in(key, 37)
    scale = 0.2 * float(TOKENS) ** 0.5
    return scale * jnp.clip(jax.random.normal(source, (RETAIN_HEADS, DK, RETAIN_VALUE_DIM), jnp.float32), -6.0, 6.0)


def draw_fox_gates(key, part):
    keys = jax.random.split(jax.random.fold_in(key, 51), 7)
    order = jax.random.permutation(keys[0], FH)
    quick = order < FH // 2
    quick_rate = 1.0 / jax.random.uniform(keys[1], (FH,), jnp.float32, 30.0, 100.0)
    slow_rate = jax.random.uniform(keys[2], (FH,), jnp.float32, 0.5, 2.0) / TOKENS
    rates = jnp.where(quick, quick_rate, slow_rate)
    blocks = TOKENS // TOK_DEV
    factor = jnp.exp(jax.random.uniform(keys[3], (blocks, 1), jnp.float32, -0.7, 0.7))
    factor = jnp.repeat(factor, TOK_DEV, axis=0)
    jitter = jax.random.uniform(keys[4], (TOKENS, FH), jnp.float32, 0.3, 1.7)
    increments = -rates[None, :] * factor * jitter
    spots = jax.random.randint(keys[5], (3,), 0, TOKENS)
    struck = jnp.any(jnp.arange(TOKENS)[:, None] == spots[None, :], axis=1)
    losses = jax.random.uniform(keys[6], (TOKENS, FH), jnp.float32, 0.22, 0.69)
    increments = increments - jnp.where(struck[:, None], losses, 0.0)
    return jnp.cumsum(increments, axis=0)


def block_scale(own_key, extent, cuts, least, top_value):
    gain, own = 1.0, jax.random.fold_in(own_key, 6)
    for axis_at, blocks in cuts:
        heights = jnp.exp(jax.random.uniform(jax.random.fold_in(own, axis_at), (blocks,), jnp.float32, least / len(cuts), top_value / len(cuts)))
        gain = gain * jnp.repeat(heights, extent[axis_at] // blocks).reshape([-1 if axis == axis_at else 1 for axis in range(len(extent))])
    return gain


def noise(key, extent, scale, limit, cuts=(), held_as=jnp.bfloat16):
    gain = block_scale(key, extent, cuts, -0.22, 0.18) if cuts else 1.0
    entries = jax.random.normal(key, extent, jnp.float32) * scale * gain
    return jnp.minimum(jnp.maximum(entries, -limit), limit).astype(held_as)


def setup_inputs(seed: int = 0, part: int = 0) -> dict:
    key_list = jax.random.split(jax.random.key(seed), 15)
    own_keys = jax.random.split(jax.random.fold_in(key_list[14], part), 15)
    return {
        "tokens": noise(own_keys[0], (TOKENS, D), 1.0, 6.0, ((0, 4), (1, 4))),
        "norm_gain": jnp.clip(1.0 + 0.18 * jax.random.normal(key_list[1], (D,), jnp.float32), 0.1, 1.9),
        "ret_query_weight": noise(key_list[2], (D, RETAIN_HEADS * DK), D ** -0.5, 0.125, ((0, 4), (1, 4))),
        "ret_key_weight": noise(key_list[3], (D, RETAIN_HEADS * DK), D ** -0.5, 0.125, ((0, 4), (1, 4))),
        "ret_value_weight": noise(key_list[4], (D, RETAIN_HEADS * RETAIN_VALUE_DIM), D ** -0.5, 0.125, ((0, 4), (1, 4))),
        "fox_query_weight": draw_fox_query_weight(jax.random.fold_in(key_list[14], 71), part),
        "fox_key_weight": noise(key_list[6], (D, FH * FD), D ** -0.5, 0.125, ((0, 4), (1, 4))),
        "fox_value_weight": noise(key_list[7], (D, FH * FD), D ** -0.5, 0.125, ((0, 4), (1, 4))),
        "ret_decay": draw_ret_decay(jax.random.fold_in(key_list[14], 71), part),
        "ret_state": draw_ret_state(jax.random.fold_in(jax.random.fold_in(key_list[14], part), 71), part),
        "head_norm_gain": jnp.clip(1.0 + 0.18 * jax.random.normal(key_list[10], (RETAIN_HEADS * RETAIN_VALUE_DIM,), jnp.float32), 0.1, 1.9),
        "fox_gates": draw_fox_gates(jax.random.fold_in(jax.random.fold_in(key_list[14], part), 71), part),
        "ret_out_weight": noise(key_list[12], (RETAIN_HEADS * RETAIN_VALUE_DIM, D), (RETAIN_HEADS * RETAIN_VALUE_DIM + FH * FD) ** -0.5, 0.1875, ((0, 4), (1, 4))),
        "fox_out_weight": noise(key_list[13], (FH * FD, D), (FH * FD // 16) ** -0.5, 1.0, ((0, 4), (1, 4))),
    }


epsilon = 1e-06
highest = lax.Precision.HIGHEST

def head_group_norm(joined_output, norm_gains):
    center = joined_output - lax.optimization_barrier(jnp.mean(joined_output, axis=-1, keepdims=True))
    spread = lax.optimization_barrier(jnp.mean(center * center, axis=-1, keepdims=True))
    normal = center * lax.rsqrt(spread + epsilon) * norm_gains.reshape(joined_output.shape[1], joined_output.shape[2])
    return normal.reshape(joined_output.shape[0], -1).astype(jnp.bfloat16)

def retention(query_rows, key_rows, value_rows, log_decay, initial, norm_gains):
    sequence_length = query_rows.shape[0]
    blocks = sequence_length // TOK_DEV
    queries = query_rows.astype(jnp.float32).reshape(blocks, TOK_DEV, RETAIN_HEADS, DK)
    keys_all = key_rows.astype(jnp.float32).reshape(blocks, TOK_DEV, RETAIN_HEADS, DK) * DK ** (-0.5)
    values_all = value_rows.astype(jnp.float32).reshape(blocks, TOK_DEV, RETAIN_HEADS, RETAIN_VALUE_DIM)
    offsets = jnp.arange(TOK_DEV, dtype=jnp.float32)
    spread = offsets[:, None] - offsets[None, :]
    within = jnp.where(spread[None] >= 0, jnp.exp(jnp.maximum(spread, 0.0)[None] * log_decay[:, None, None]), 0.0)
    leading = jnp.exp((offsets + 1.0)[:, None] * log_decay[None, :])
    trailing = jnp.exp((TOK_DEV - 1.0 - offsets)[:, None] * log_decay[None, :])
    blockwise = jnp.exp(TOK_DEV * log_decay)

    def advance(memory, inputs):
        qblock, kblock, vblock = inputs
        scores = jnp.einsum('ihd,jhd->hij', qblock, kblock, precision=highest) * within
        inner_value = jnp.einsum('hij,jhe->ihe', scores, vblock, precision=highest)
        carried_state = jnp.einsum('ihd,hde->ihe', qblock, memory, precision=highest) * leading[:, :, None]
        summary = jnp.einsum('jhd,jhe->hde', kblock * trailing[:, :, None], vblock, precision=highest)
        return (memory * blockwise[:, None, None] + summary, inner_value + carried_state)
    _, output_rows = lax.scan(advance, initial, (queries, keys_all, values_all))
    return head_group_norm(output_rows.reshape(sequence_length, RETAIN_HEADS, RETAIN_VALUE_DIM), norm_gains)

def forgetting(query_rows, key_rows, value_rows, gates):
    sequence_length = query_rows.shape[0]
    queries = query_rows.astype(jnp.float32).reshape(sequence_length, FH, FD)
    keys_all = key_rows.astype(jnp.float32).reshape(sequence_length, FH, FD)
    values_all = value_rows.astype(jnp.float32).reshape(sequence_length, FH, FD)
    key_gates = gates.T
    key_pos = jnp.arange(sequence_length, dtype=jnp.int32)

    def block(number):
        first = (number * TOK_DEV).astype(jnp.int32)
        qblock = lax.dynamic_slice_in_dim(queries, first, TOK_DEV, 0)
        own_gates = lax.dynamic_slice_in_dim(key_gates, first, TOK_DEV, 1)
        scores = jnp.einsum('qhd,khd->hqk', qblock, keys_all) * FD ** (-0.5)
        scores = scores + own_gates[:, :, None] - key_gates[:, None, :]
        query_pos = first + jnp.arange(TOK_DEV, dtype=jnp.int32)
        scores = jnp.where(key_pos[None, None, :] <= query_pos[None, :, None], scores, -jnp.inf)
        highest_score = lax.optimization_barrier(jnp.max(scores, axis=-1, keepdims=True))
        weights = jnp.exp(scores - highest_score)
        totals = lax.optimization_barrier(jnp.sum(weights, axis=-1))
        rounded = lax.optimization_barrier(weights.astype(jnp.bfloat16)).astype(jnp.float32)
        weighted = jnp.einsum('hqk,khd->hqd', rounded, values_all)
        result = weighted / totals[:, :, None]
        return jnp.transpose(result, (1, 0, 2)).reshape(TOK_DEV, FH * FD).astype(jnp.bfloat16)
    pieces = lax.map(block, jnp.arange(sequence_length // TOK_DEV, dtype=jnp.int32))
    return pieces.reshape(sequence_length, FH * FD)

def reference(tokens, norm_gain, ret_query_weight, ret_key_weight, ret_value_weight, fox_query_weight, fox_key_weight, fox_value_weight, ret_decay, ret_state, head_norm_gain, fox_gates, ret_out_weight, fox_out_weight):
    widened = tokens.astype(jnp.float32)
    normed = (widened * lax.rsqrt(lax.optimization_barrier(jnp.mean(widened * widened, axis=-1, keepdims=True)) + epsilon) * norm_gain).astype(jnp.bfloat16)
    matrices = (ret_query_weight, ret_key_weight, ret_value_weight, fox_query_weight, fox_key_weight, fox_value_weight)
    ret_query, ret_key, ret_value, fox_query, fox_key, fox_value = [jnp.dot(normed, matrix, preferred_element_type=jnp.float32).astype(jnp.bfloat16) for matrix in matrices]
    retention_mixed = retention(ret_query, ret_key, ret_value, ret_decay, ret_state, head_norm_gain)
    fox_mix = forgetting(fox_query, fox_key, fox_value, fox_gates)
    ret_width = RETAIN_HEADS * RETAIN_VALUE_DIM // N_TP
    fox_width = FH * FD // N_TP
    summed = jnp.zeros((tokens.shape[0], D), jnp.float32)
    for member in range(N_TP):
        portion = jnp.dot(retention_mixed[:, member * ret_width:(member + 1) * ret_width], ret_out_weight[member * ret_width:(member + 1) * ret_width], preferred_element_type=jnp.float32)
        portion = portion + jnp.dot(fox_mix[:, member * fox_width:(member + 1) * fox_width], fox_out_weight[member * fox_width:(member + 1) * fox_width], preferred_element_type=jnp.float32)
        summed = summed + lax.optimization_barrier(portion.astype(jnp.bfloat16)).astype(jnp.float32)
    return summed.astype(jnp.bfloat16)
```

```python
import functools

import jax
import jax.numpy as jnp
from jax import lax
from jax.experimental import pallas as pl
from jax.experimental.pallas import tpu as pltpu
from jax.sharding import PartitionSpec as P

epsilon = 1e-06
highest = lax.Precision.HIGHEST
NT = (((1,), (1,)), ((), ()))
TN = (((0,), (0,)), ((), ()))


def rdma(src, dst, send_sem, recv_sem, **target):
    return pltpu.make_async_remote_copy(
        src_ref=src,
        dst_ref=dst,
        send_sem=send_sem,
        recv_sem=recv_sem,
        device_id=target,
        device_id_type=pl.DeviceIdType.MESH,
    )


class LineGather:
    def __init__(self, own, buf, sems, n, n_grp, me, g, chunks):
        self.own, self.buf, self.n, self.n_grp, self.me, self.g = own, buf, n, n_grp, me, g
        self.up, self.down, self.zr, self.ys, self.yr, self.loc = sems
        self.rows = own.shape[0]
        self.part = self.rows // n_grp
        self.chunks = chunks
        self.step = self.part // chunks

    def piece(self, part, src, c):
        start = pl.multiple_of(src * self.rows + part * self.part + c * self.step, self.step)
        return self.buf.at[pl.ds(start, self.step)]

    def own_piece(self, c):
        start = pl.multiple_of(self.g * self.part + c * self.step, self.step)
        return self.own.at[pl.ds(start, self.step)]

    def hop(self, sems, to, src, c, first=False):
        here = self.own_piece(c) if first else self.piece(self.g, src, c)
        at = src * self.chunks + c
        return rdma(here, self.piece(self.g, src, c), sems.at[at], self.zr.at[at], sp=to)

    def side(self, d, src, c):
        at = ((d - 1) * self.n + src) * self.chunks + c
        here = self.piece(self.g, src, c)
        return rdma(here, here, self.ys.at[at], self.yr.at[at], grp=lax.rem(self.g + d, self.n_grp))

    def side_in(self, d, src, c):
        at = ((d - 1) * self.n + src) * self.chunks + c
        part = lax.rem(self.g + self.n_grp - d, self.n_grp)
        here = self.piece(part, src, c)
        return rdma(here, here, self.ys.at[at], self.yr.at[at], grp=part)

    def local(self):
        start = pl.multiple_of(self.me * self.rows, self.rows)
        return pltpu.make_async_copy(self.own, self.buf.at[pl.ds(start, self.rows)], self.loc)

    def start(self):
        me, n = self.me, self.n
        for c in range(self.chunks):

            @pl.when(me + 1 < n)
            def _():
                self.hop(self.up, me + 1, me, c, True).start()

            @pl.when(me >= 1)
            def _():
                self.hop(self.down, me - 1, me, c, True).start()

        self.local().start()

    def relay(self):
        me, n = self.me, self.n

        def step(k, _):
            for c in range(self.chunks):
                for src, sems, to in ((me - k, self.up, me + 1), (me + k, self.down, me - 1)):

                    @pl.when((src >= 0) & (src < n))
                    def _(src=src, sems=sems, to=to):
                        self.hop(sems, me, src, c).wait_recv()

                        @pl.when((to >= 0) & (to < n))
                        def _():
                            self.hop(sems, to, src, c).start()

                        for d in range(1, self.n_grp):
                            self.side(d, src, c).start()

            return 0

        lax.fori_loop(1, n, step, 0)

    def arrive(self):
        self.local().wait()

        def step(k, _):
            src = lax.rem(self.me + k, self.n)
            for c in range(self.chunks):
                for d in range(1, self.n_grp):
                    self.side_in(d, src, c).wait_recv()
            return 0

        lax.fori_loop(1, self.n, step, 0)

    def finish(self):
        me, n = self.me, self.n

        def step(src, _):
            for c in range(self.chunks):

                @pl.when((src <= me) & (me + 1 < n))
                def _():
                    self.hop(self.up, me, src, c).wait_send()

                @pl.when((src >= me) & (me >= 1))
                def _():
                    self.hop(self.down, me, src, c).wait_send()

                @pl.when(src != me)
                def _():
                    for d in range(1, self.n_grp):
                        self.side(d, src, c).wait_send()

            return 0

        lax.fori_loop(0, n, step, 0)


def kernel(
    size,
    tok_ref,
    gain_ref,
    w_ref,
    decay_ref,
    state_ref,
    hgain_ref,
    gates_ref,
    gates_t_ref,
    wout_ref,
    out_ref,
    tok_buf,
    w_buf,
    wout_buf,
    norm_buf,
    proj_buf,
    kv_buf,
    sum_buf,
    mix_buf,
    rs_send,
    rs_buf,
    tok_s,
    tok_r,
    tok_loc,
    kv_s,
    kv_r,
    sum_s,
    sum_r,
    rs_s,
    rs_r,
    *gather_sems,
):
    n, n_tp, n_grp, hr, dk, vd, fh, fd, chunks, out_chunks = size
    me, t, g = lax.axis_index("sp"), lax.axis_index("tp"), lax.axis_index("grp")
    rows = tok_ref.shape[0]
    feats = tok_ref.shape[1]
    weights = LineGather(w_ref, w_buf, gather_sems[:6], n, n_grp, me, g, chunks)
    outs = LineGather(wout_ref, wout_buf, gather_sems[6:], n, n_grp, me, g, out_chunks)

    barrier = pltpu.get_barrier_semaphore()

    def greet(**target):
        pl.semaphore_signal(barrier, inc=1, device_id=target, device_id_type=pl.DeviceIdType.MESH)

    has_up, has_down = me + 1 < n, me >= 1
    for d in range(1, n_tp):
        greet(tp=lax.rem(t + d, n_tp))
    for d in range(1, n_grp):
        greet(grp=lax.rem(g + d, n_grp))

    @pl.when(has_up)
    def _():
        greet(sp=me + 1)

    @pl.when(has_down)
    def _():
        greet(sp=me - 1)

    count = n_tp - 1 + n_grp - 1 + has_up.astype(jnp.int32) + has_down.astype(jnp.int32)
    pl.semaphore_wait(barrier, count)

    weights.start()

    def tok_copy(d):
        return rdma(tok_ref, tok_buf.at[t], tok_s.at[d - 1], tok_r.at[d - 1], tp=lax.rem(t + d, n_tp))

    def tok_in(d):
        src = lax.rem(t + n_tp - d, n_tp)
        return rdma(tok_ref, tok_buf.at[src], tok_s.at[d - 1], tok_r.at[d - 1], tp=src)

    tok_local = pltpu.make_async_copy(tok_ref, tok_buf.at[t], tok_loc)
    for d in range(1, n_tp):
        tok_copy(d).start()
    tok_local.start()

    weights.relay()
    outs.start()

    tok_local.wait()
    for d in range(1, n_tp):
        tok_in(d).wait_recv()
    squares = jnp.zeros((rows, 1), jnp.float32)
    for i in range(n_tp):
        part = tok_buf[i].astype(jnp.float32)
        squares = squares + jnp.sum(part * part, axis=-1, keepdims=True)
    scale = lax.rsqrt(squares * (1.0 / (n_tp * feats)) + epsilon)
    for i in range(n_tp):
        part = tok_buf[i].astype(jnp.float32)
        cols = slice(i * feats, (i + 1) * feats)
        norm_buf[:, cols] = (part * scale * gain_ref[:, cols]).astype(jnp.bfloat16)

    outs.relay()
    weights.arrive()

    fox_kv = hr * (2 * dk + vd) + fh * fd
    kv_width = 2 * fh * fd
    result = jnp.dot(norm_buf[...], w_buf[...], preferred_element_type=jnp.float32)
    proj_buf[...] = result.astype(jnp.bfloat16)
    kv_buf[me] = proj_buf[:, fox_kv : fox_kv + kv_width]

    def kv_copy(src):
        return rdma(kv_buf.at[src], kv_buf.at[src], kv_s.at[src], kv_r.at[src], sp=jnp.minimum(me + 1, n - 1))

    def sum_copy(src):
        return rdma(sum_buf.at[src], sum_buf.at[src], sum_s.at[src], sum_r.at[src], sp=jnp.minimum(me + 1, n - 1))

    @pl.when(has_up)
    def _():
        kv_copy(me).start()

    key_scale = dk ** (-0.5)
    position = lax.broadcasted_iota(jnp.int32, (rows, 1), 0).astype(jnp.float32)
    rq, rk, rv = [], [], []
    for h in range(hr):
        rq.append(proj_buf[:, h * dk : (h + 1) * dk])
        rk.append(proj_buf[:, (hr + h) * dk : (hr + h + 1) * dk])
        rv.append(proj_buf[:, 2 * hr * dk + h * vd : 2 * hr * dk + (h + 1) * vd])
        keys = rk[h].astype(jnp.float32) * key_scale
        trailing = jnp.exp((rows - 1.0 - position) * decay_ref[h])
        sum_buf[me, h] = lax.dot_general(
            keys * trailing, rv[h].astype(jnp.float32), TN, precision=highest, preferred_element_type=jnp.float32
        )

    @pl.when(has_up)
    def _():
        sum_copy(me).start()

    row_id = lax.broadcasted_iota(jnp.int32, (rows, rows), 0)
    col_id = lax.broadcasted_iota(jnp.int32, (rows, rows), 1)
    causal = col_id <= row_id
    fq = [proj_buf[:, hr * (2 * dk + vd) + h * fd : hr * (2 * dk + vd) + (h + 1) * fd] for h in range(fh)]
    own_rows = pl.ds(pl.multiple_of(me * rows, rows), rows)
    own_gates = gates_ref[own_rows, :]

    def attend(src, current, diagonal):
        key_cols = pl.ds(pl.multiple_of(src * rows, rows), rows)
        following = []
        for h in range(fh):
            top, total, weighted = current[h]
            k = kv_buf[src, :, h * fd : (h + 1) * fd]
            v = kv_buf[src, :, (fh + h) * fd : (fh + h + 1) * fd]
            logits = lax.dot_general(fq[h], k, NT, preferred_element_type=jnp.float32) * fd ** (-0.5)
            logits = logits + own_gates[:, h : h + 1] - gates_t_ref[h : h + 1, key_cols]
            if diagonal:
                logits = jnp.where(causal, logits, -jnp.inf)
            top_new = jnp.maximum(top, jnp.max(logits, axis=-1, keepdims=True))
            p = jnp.exp(logits - top_new)
            rescale = jnp.exp(top - top_new)
            total = total * rescale + jnp.sum(p, axis=-1, keepdims=True)
            weighted = weighted * rescale + jnp.dot(p.astype(jnp.bfloat16), v, preferred_element_type=jnp.float32)
            following.append((top_new, total, weighted))
        return tuple(following)

    start = tuple(
        (
            jnp.full((rows, 1), -1e30, jnp.float32),
            jnp.zeros((rows, 1), jnp.float32),
            jnp.zeros((rows, fd), jnp.float32),
        )
        for _ in range(fh)
    )
    current = attend(me, start, True)

    inner = []
    distance = jnp.maximum(row_id - col_id, 0).astype(jnp.float32)
    for h in range(hr):
        scores = lax.dot_general(rq[h], rk[h], NT, preferred_element_type=jnp.float32) * key_scale
        scores = jnp.where(causal, scores * jnp.exp(distance * decay_ref[h]), 0.0)
        inner.append(
            jnp.dot(scores, rv[h].astype(jnp.float32), precision=highest, preferred_element_type=jnp.float32)
        )

    offset = (me * rows).astype(jnp.float32)
    lone = jnp.zeros((dk, vd), jnp.float32)
    entering = tuple(jnp.exp(lone + offset * decay_ref[h]) * state_ref[h] for h in range(hr))

    def earlier(k, carry):
        current, entering = carry
        src = me - k
        kv_copy(src).wait_recv()

        @pl.when(has_up)
        def _():
            kv_copy(src).start()

        sum_copy(src).wait_recv()

        @pl.when(has_up)
        def _():
            sum_copy(src).start()

        gap = ((k - 1) * rows).astype(jnp.float32)
        entering = tuple(
            entering[h] + jnp.exp(lone + gap * decay_ref[h]) * sum_buf[src, h] for h in range(hr)
        )
        return attend(src, current, False), entering

    current, entering = lax.fori_loop(1, me + 1, earlier, (current, entering))

    for h in range(hr):
        leading = jnp.exp((position + 1.0) * decay_ref[h])
        carried = jnp.dot(
            rq[h].astype(jnp.float32), entering[h], precision=highest, preferred_element_type=jnp.float32
        )
        raw = inner[h] + carried * leading
        center = raw - jnp.mean(raw, axis=-1, keepdims=True)
        variance = jnp.mean(center * center, axis=-1, keepdims=True)
        cols = slice(h * vd, (h + 1) * vd)
        mix_buf[:, cols] = (center * lax.rsqrt(variance + epsilon) * hgain_ref[:, cols]).astype(jnp.bfloat16)
    for h in range(fh):
        top, total, weighted = current[h]
        cols = slice(hr * vd + h * fd, hr * vd + (h + 1) * fd)
        mix_buf[:, cols] = (weighted / total).astype(jnp.bfloat16)

    outs.arrive()
    block = rows // n_tp

    def rs_copy(d):
        return rdma(
            rs_send.at[d - 1], rs_buf.at[d - 1], rs_s.at[d - 1], rs_r.at[d - 1], tp=lax.rem(t + d, n_tp)
        )

    def partial(owner):
        mine = mix_buf[pl.ds(pl.multiple_of(owner * block, block), block), :]
        return lax.dot_general(mine, wout_buf[...], NT, preferred_element_type=jnp.float32).astype(jnp.bfloat16)

    for d in reversed(range(1, n_tp)):
        rs_send[d - 1] = partial(lax.rem(t + d, n_tp))
        rs_copy(d).start()
    summed = partial(t).astype(jnp.float32)
    for d in range(1, n_tp):
        rs_copy(d).wait_recv()
        summed = summed + rs_buf[d - 1].astype(jnp.float32)
    out_ref[...] = summed.astype(jnp.bfloat16)

    for d in range(1, n_tp):
        tok_copy(d).wait_send()
        rs_copy(d).wait_send()
    weights.finish()
    outs.finish()

    @pl.when(has_up)
    def _():
        def step(src, _):
            kv_copy(src).wait_send()
            sum_copy(src).wait_send()
            return 0

        lax.fori_loop(0, me + 1, step, 0)


def local(
    n,
    n_tp,
    n_grp,
    tokens,
    norm_gain,
    ret_query_weight,
    ret_key_weight,
    ret_value_weight,
    fox_query_weight,
    fox_key_weight,
    fox_value_weight,
    ret_decay,
    ret_state,
    head_norm_gain,
    fox_gates,
    ret_out_weight,
    fox_out_weight,
):
    rows, feats = tokens.shape
    hr, dk, vd = ret_state.shape
    fh = fox_gates.shape[1]
    fd = fox_query_weight.shape[1] // fh
    joined = jnp.concatenate(
        (
            ret_query_weight,
            ret_key_weight,
            ret_value_weight,
            fox_query_weight,
            fox_key_weight,
            fox_value_weight,
        ),
        axis=1,
    )
    out_joined = jnp.concatenate((ret_out_weight, fox_out_weight), axis=0).T
    width, depth = joined.shape[1], out_joined.shape[1]
    columns = out_joined.shape[0] * n

    def chunks_of(count):
        part = count // n_grp
        return 2 if part % 32 == 0 else 1

    chunks, out_chunks = chunks_of(joined.shape[0]), chunks_of(out_joined.shape[0])
    dma = pltpu.SemaphoreType.DMA

    def gather_sems(parts):
        return [
            dma((n * parts,)),
            dma((n * parts,)),
            dma((n * parts,)),
            dma((max(n_grp - 1, 1) * n * parts,)),
            dma((max(n_grp - 1, 1) * n * parts,)),
            dma,
        ]

    vmem = pl.BlockSpec(memory_space=pltpu.VMEM)
    smem = pl.BlockSpec(memory_space=pltpu.SMEM)
    size = (n, n_tp, n_grp, hr, dk, vd, fh, fd, chunks, out_chunks)
    block = rows // n_tp
    peers = max(n_tp - 1, 1)
    return pl.pallas_call(
        functools.partial(kernel, size),
        out_shape=jax.ShapeDtypeStruct((block, columns), jnp.bfloat16),
        in_specs=[vmem, vmem, vmem, smem, vmem, vmem, vmem, vmem, vmem],
        out_specs=vmem,
        scratch_shapes=[
            pltpu.VMEM((n_tp, rows, feats), jnp.bfloat16),
            pltpu.VMEM((n * joined.shape[0], width), jnp.bfloat16),
            pltpu.VMEM((columns, depth), jnp.bfloat16),
            pltpu.VMEM((rows, n_tp * feats), jnp.bfloat16),
            pltpu.VMEM((rows, width), jnp.bfloat16),
            pltpu.VMEM((n, rows, 2 * fh * fd), jnp.bfloat16),
            pltpu.VMEM((n, hr, dk, vd), jnp.float32),
            pltpu.VMEM((rows, depth), jnp.bfloat16),
            pltpu.VMEM((peers, block, columns), jnp.bfloat16),
            pltpu.VMEM((peers, block, columns), jnp.bfloat16),
            dma((peers,)),
            dma((peers,)),
            dma,
            dma((n,)),
            dma((n,)),
            dma((n,)),
            dma((n,)),
            dma((peers,)),
            dma((peers,)),
        ]
        + gather_sems(chunks)
        + gather_sems(out_chunks),
        compiler_params=pltpu.CompilerParams(
            collective_id=0, has_side_effects=True, vmem_limit_bytes=48 * 1024 * 1024
        ),
        name="layer",
    )(
        tokens,
        norm_gain[None, :],
        joined,
        ret_decay,
        ret_state,
        head_norm_gain[None, :],
        fox_gates,
        fox_gates.T,
        out_joined,
    )


def solution(mesh):
    placed = (
        P(("grp", "sp"), "tp"),
        P(),
        P("sp", "tp"),
        P("sp", "tp"),
        P("sp", "tp"),
        P("sp", "tp"),
        P("sp", "tp"),
        P("sp", "tp"),
        P("tp"),
        P(("grp", "tp"), None, None),
        P("tp"),
        P("grp", "tp"),
        P("tp", "sp"),
        P("tp", "sp"),
    )
    body = functools.partial(local, mesh.shape["sp"], mesh.shape["tp"], mesh.shape["grp"])
    return jax.shard_map(
        body, mesh=mesh, in_specs=placed, out_specs=P(("grp", "sp", "tp"), None), check_vma=False
    )
```

```python
import functools

import jax
import jax.numpy as jnp
from jax import lax
from jax.experimental import pallas as pl
from jax.experimental.pallas import tpu as pltpu
from jax.sharding import PartitionSpec as P

epsilon = 1e-06
highest = lax.Precision.HIGHEST
NT = (((1,), (1,)), ((), ()))
TN = (((0,), (0,)), ((), ()))


def rdma(src, dst, send_sem, recv_sem, **target):
    return pltpu.make_async_remote_copy(
        src_ref=src,
        dst_ref=dst,
        send_sem=send_sem,
        recv_sem=recv_sem,
        device_id=target,
        device_id_type=pl.DeviceIdType.MESH,
    )


class LineGather:
    def __init__(self, owns, place, sems, n, n_grp, me, g):
        self.owns, self.place, self.n, self.n_grp, self.me, self.g = owns, place, n, n_grp, me, g
        self.up, self.down, self.zr, self.ys, self.yr, self.loc = sems
        self.arrays = len(owns)
        self.rows = owns[0].shape[0]
        self.step = self.rows // n_grp

    def piece(self, part, src, c):
        return self.place(src, c, part * self.step, self.step)

    def own_piece(self, c):
        return self.owns[c].at[pl.ds(pl.multiple_of(self.g * self.step, self.step), self.step)]

    def hop(self, sems, to, src, c, first=False):
        here = self.own_piece(c) if first else self.piece(self.g, src, c)
        at = src * self.arrays + c
        return rdma(here, self.piece(self.g, src, c), sems.at[at], self.zr.at[at], sp=to)

    def side(self, d, src, c):
        at = ((d - 1) * self.n + src) * self.arrays + c
        here = self.piece(self.g, src, c)
        return rdma(here, here, self.ys.at[at], self.yr.at[at], grp=lax.rem(self.g + d, self.n_grp))

    def side_in(self, d, src, c):
        at = ((d - 1) * self.n + src) * self.arrays + c
        part = lax.rem(self.g + self.n_grp - d, self.n_grp)
        here = self.piece(part, src, c)
        return rdma(here, here, self.ys.at[at], self.yr.at[at], grp=part)

    def local(self, c):
        return pltpu.make_async_copy(self.owns[c], self.place(self.me, c, 0, self.rows), self.loc.at[c])

    def start(self):
        me, n = self.me, self.n
        for c in range(self.arrays):

            @pl.when(me + 1 < n)
            def _():
                self.hop(self.up, me + 1, me, c, True).start()

            @pl.when(me >= 1)
            def _():
                self.hop(self.down, me - 1, me, c, True).start()

        for c in range(self.arrays):
            self.local(c).start()

    def relay(self, k):
        me, n = self.me, self.n
        for c in range(self.arrays):
            for src, sems, to in ((me - k, self.up, me + 1), (me + k, self.down, me - 1)):

                @pl.when((src >= 0) & (src < n))
                def _(src=src, sems=sems, to=to):
                    self.hop(sems, me, src, c).wait_recv()

                    @pl.when((to >= 0) & (to < n))
                    def _():
                        self.hop(sems, to, src, c).start()

                    for d in range(1, self.n_grp):
                        self.side(d, src, c).start()

    def arrive_shard(self, src, arrays):
        for c in arrays:
            for d in range(1, self.n_grp):
                self.side_in(d, src, c).wait_recv()

    def arrive(self, arrays):
        for c in arrays:
            self.local(c).wait()

        def step(k, _):
            self.arrive_shard(lax.rem(self.me + k, self.n), arrays)
            return 0

        lax.fori_loop(1, self.n, step, 0)

    def finish(self):
        me, n = self.me, self.n

        def step(src, _):
            for c in range(self.arrays):

                @pl.when((src <= me) & (me + 1 < n))
                def _():
                    self.hop(self.up, me, src, c).wait_send()

                @pl.when((src >= me) & (me >= 1))
                def _():
                    self.hop(self.down, me, src, c).wait_send()

                @pl.when(src != me)
                def _():
                    for d in range(1, self.n_grp):
                        self.side(d, src, c).wait_send()

            return 0

        lax.fori_loop(0, n, step, 0)


def kernel(
    size,
    tok_ref,
    gain_ref,
    wq_ref,
    wk_ref,
    wrv_ref,
    wfq_ref,
    wfk_ref,
    wfv_ref,
    decay_ref,
    state_ref,
    hgain_ref,
    gates_ref,
    ret_out_ref,
    fox_out_ref,
    out_ref,
    tok_buf,
    qk_own,
    w_buf,
    wout_buf,
    norm_buf,
    proj_buf,
    kv_buf,
    sum_buf,
    mix_buf,
    rs_send,
    rs_buf,
    top_buf,
    total_buf,
    weighted_buf,
    tok_s,
    tok_r,
    tok_loc,
    kv_s,
    kv_r,
    sum_s,
    sum_r,
    rs_s,
    rs_r,
    *gather_sems,
):
    n, n_tp, n_grp, hr, dk, vd, fh, fd, direct = size
    me, t, g = lax.axis_index("sp"), lax.axis_index("tp"), lax.axis_index("grp")
    rows, feats = tok_ref.shape
    owns = [wfk_ref, wfv_ref, wfq_ref, wrv_ref, qk_own]
    starts = [0]
    for own in owns:
        starts.append(starts[-1] + own.shape[1])
    shard = qk_own.shape[0]

    def weight_place(src, c, first, count):
        start = pl.multiple_of(src * shard + first, count)
        return w_buf.at[pl.ds(start, count), starts[c] : starts[c + 1]]

    depth = mix_buf.shape[1] // 2
    out_cols = ret_out_ref.shape[1] if direct else ret_out_ref.shape[0]

    def out_place(src, c, first, count):
        if direct:
            start = pl.multiple_of(c * depth + first, count)
            return wout_buf.at[pl.ds(start, count), pl.ds(pl.multiple_of(src * out_cols, out_cols), out_cols)]
        start = pl.multiple_of(src * out_cols + first, count)
        return wout_buf.at[pl.ds(start, count), c * depth : (c + 1) * depth]

    weights = LineGather(owns, weight_place, gather_sems[:6], n, n_grp, me, g)
    outs = LineGather([ret_out_ref, fox_out_ref], out_place, gather_sems[6:], n, n_grp, me, g)

    barrier = pltpu.get_barrier_semaphore()

    def greet(**target):
        pl.semaphore_signal(barrier, inc=1, device_id=target, device_id_type=pl.DeviceIdType.MESH)

    has_up, has_down = me + 1 < n, me >= 1
    for d in range(1, n_tp):
        greet(tp=lax.rem(t + d, n_tp))
    for d in range(1, n_grp):
        greet(grp=lax.rem(g + d, n_grp))

    @pl.when(has_up)
    def _():
        greet(sp=me + 1)

    @pl.when(has_down)
    def _():
        greet(sp=me - 1)

    turned = jnp.concatenate((wq_ref[...], wk_ref[...]), axis=0).astype(jnp.float32)
    qk_own[...] = turned.T.astype(jnp.bfloat16)

    count = n_tp - 1 + n_grp - 1 + has_up.astype(jnp.int32) + has_down.astype(jnp.int32)
    pl.semaphore_wait(barrier, count)

    def tok_copy(d):
        return rdma(tok_ref, tok_buf.at[t], tok_s.at[d - 1], tok_r.at[d - 1], tp=lax.rem(t + d, n_tp))

    def tok_in(d):
        src = lax.rem(t + n_tp - d, n_tp)
        return rdma(tok_ref, tok_buf.at[src], tok_s.at[d - 1], tok_r.at[d - 1], tp=src)

    weights.start()
    tok_local = pltpu.make_async_copy(tok_ref, tok_buf.at[t], tok_loc)
    for d in range(1, n_tp):
        tok_copy(d).start()
    tok_local.start()

    def weight_step(k, _):
        weights.relay(k)
        return 0

    lax.fori_loop(1, n, weight_step, 0)
    outs.start()

    tok_local.wait()
    for d in range(1, n_tp):
        tok_in(d).wait_recv()
    squares = jnp.zeros((rows, 1), jnp.float32)
    for i in range(n_tp):
        part = tok_buf[i].astype(jnp.float32)
        squares = squares + jnp.sum(part * part, axis=-1, keepdims=True)
    scale = lax.rsqrt(squares * (1.0 / (n_tp * feats)) + epsilon)
    for i in range(n_tp):
        part = tok_buf[i].astype(jnp.float32)
        cols = slice(i * feats, (i + 1) * feats)
        norm_buf[:, cols] = (part * scale * gain_ref[:, cols]).astype(jnp.bfloat16)

    def kv_copy(src):
        return rdma(kv_buf.at[src], kv_buf.at[src], kv_s.at[src], kv_r.at[src], sp=jnp.minimum(me + 1, n - 1))

    def sum_copy(src):
        return rdma(sum_buf.at[src], sum_buf.at[src], sum_s.at[src], sum_r.at[src], sp=jnp.minimum(me + 1, n - 1))

    weights.arrive((0, 1))
    kv_buf[me] = jnp.dot(
        norm_buf[...], w_buf[:, : starts[2]], preferred_element_type=jnp.float32
    ).astype(jnp.bfloat16)

    @pl.when(has_up)
    def _():
        kv_copy(me).start()

    if n > 1:
        outs.relay(1)
    weights.arrive((2, 3, 4))
    proj_buf[...] = jnp.dot(
        norm_buf[...], w_buf[:, starts[2] :], preferred_element_type=jnp.float32
    ).astype(jnp.bfloat16)
    rv_at, rq_at = starts[3] - starts[2], starts[4] - starts[2]

    key_scale = dk ** (-0.5)
    position = lax.broadcasted_iota(jnp.int32, (rows, 1), 0).astype(jnp.float32)
    rq, rk, rv = [], [], []
    for h in range(hr):
        rq.append(proj_buf[:, rq_at + h * dk : rq_at + (h + 1) * dk])
        rk.append(proj_buf[:, rq_at + (hr + h) * dk : rq_at + (hr + h + 1) * dk])
        rv.append(proj_buf[:, rv_at + h * vd : rv_at + (h + 1) * vd])
        keys = rk[h].astype(jnp.float32) * key_scale
        trailing = jnp.exp((rows - 1.0 - position) * decay_ref[h])
        sum_buf[me, h] = lax.dot_general(
            keys * trailing, rv[h].astype(jnp.float32), TN, precision=highest, preferred_element_type=jnp.float32
        )

    @pl.when(has_up)
    def _():
        sum_copy(me).start()

    row_id = lax.broadcasted_iota(jnp.int32, (rows, rows), 0)
    col_id = lax.broadcasted_iota(jnp.int32, (rows, rows), 1)
    causal = col_id <= row_id
    own_cols = pl.ds(pl.multiple_of(me * rows, rows), rows)
    own_gates = [
        jnp.sum(jnp.where(row_id == col_id, gates_ref[h : h + 1, own_cols], 0.0), axis=1, keepdims=True)
        for h in range(fh)
    ]

    def attend(src, diagonal):
        key_cols = pl.ds(pl.multiple_of(src * rows, rows), rows)
        for h in range(fh):
            query = proj_buf[:, h * fd : (h + 1) * fd]
            k = kv_buf[src, :, h * fd : (h + 1) * fd]
            v = kv_buf[src, :, (fh + h) * fd : (fh + h + 1) * fd]
            logits = lax.dot_general(query, k, NT, preferred_element_type=jnp.float32) * fd ** (-0.5)
            logits = logits + own_gates[h] - gates_ref[h : h + 1, key_cols]
            if diagonal:
                logits = jnp.where(causal, logits, -jnp.inf)
            top_new = jnp.max(logits, axis=-1, keepdims=True)
            if not diagonal:
                top = top_buf[h]
                top_new = jnp.maximum(top, top_new)
            p = jnp.exp(logits - top_new)
            total = jnp.sum(p, axis=-1, keepdims=True)
            weighted = jnp.dot(p.astype(jnp.bfloat16), v, preferred_element_type=jnp.float32)
            if not diagonal:
                rescale = jnp.exp(top - top_new)
                total = total_buf[h] * rescale + total
                weighted = weighted_buf[h] * rescale + weighted
            top_buf[h] = top_new
            total_buf[h] = total
            weighted_buf[h] = weighted

    def forward(k):
        src = me - k

        @pl.when(src >= 0)
        def _():
            kv_copy(src).wait_recv()

            @pl.when(has_up)
            def _():
                kv_copy(src).start()

            sum_copy(src).wait_recv()

            @pl.when(has_up)
            def _():
                sum_copy(src).start()

    attend(me, True)

    offset = (me * rows).astype(jnp.float32)
    lone = jnp.zeros((dk, vd), jnp.float32)

    def step(k, entering):
        src = me - k
        forward(k)

        @pl.when(k + 1 < n)
        def _():
            outs.relay(k + 1)

        @pl.when(src >= 0)
        def _():
            attend(src, False)

        gap = ((k - 1) * rows).astype(jnp.float32)
        there = jnp.maximum(src, 0)
        return tuple(
            entering[h]
            + jnp.where(src >= 0, jnp.exp(lone + gap * decay_ref[h]) * sum_buf[there, h], 0.0)
            for h in range(hr)
        )

    entering = tuple(jnp.exp(lone + offset * decay_ref[h]) * state_ref[h] for h in range(hr))
    entering = lax.fori_loop(1, n, step, entering)

    distance = jnp.maximum(row_id - col_id, 0).astype(jnp.float32)
    for h in range(hr):
        scores = lax.dot_general(rq[h], rk[h], NT, preferred_element_type=jnp.float32) * key_scale
        scores = jnp.where(causal, scores * jnp.exp(distance * decay_ref[h]), 0.0)
        inner = jnp.dot(scores, rv[h].astype(jnp.float32), precision=highest, preferred_element_type=jnp.float32)
        leading = jnp.exp((position + 1.0) * decay_ref[h])
        carried = jnp.dot(
            rq[h].astype(jnp.float32), entering[h], precision=highest, preferred_element_type=jnp.float32
        )
        raw = inner + carried * leading
        center = raw - jnp.mean(raw, axis=-1, keepdims=True)
        variance = jnp.mean(center * center, axis=-1, keepdims=True)
        cols = slice(h * vd, (h + 1) * vd)
        mix_buf[:, cols] = (center * lax.rsqrt(variance + epsilon) * hgain_ref[:, cols]).astype(jnp.bfloat16)
    for h in range(fh):
        cols = slice(hr * vd + h * fd, hr * vd + (h + 1) * fd)
        mix_buf[:, cols] = (weighted_buf[h] / total_buf[h]).astype(jnp.bfloat16)

    block = rows // n_tp
    columns = rs_send.shape[1]
    wide = out_cols if direct else columns
    pieces = columns // wide
    mine = pl.ds(pl.multiple_of(t * block, block), block)

    def rs_copy(d, piece):
        to = lax.rem(t + d, n_tp)
        cols = pl.ds(pl.multiple_of(piece * wide, wide), wide)
        at = (d - 1) * pieces + piece
        return rdma(
            rs_send.at[pl.ds(pl.multiple_of(to * block, block), block), cols],
            rs_buf.at[d - 1, :, cols],
            rs_s.at[at],
            rs_r.at[at],
            tp=to,
        )

    def project(piece):
        cols = pl.ds(pl.multiple_of(piece * wide, wide), wide)
        if direct:
            value = jnp.dot(mix_buf[...], wout_buf[:, cols], preferred_element_type=jnp.float32)
        else:
            value = lax.dot_general(mix_buf[...], wout_buf[...], NT, preferred_element_type=jnp.float32)
        rs_send[:, cols] = value.astype(jnp.bfloat16)
        for d in range(1, n_tp):
            rs_copy(d, piece).start()

    if direct:
        for c in range(2):
            outs.local(c).wait()
        project(me)

        def out_step(k, _):
            for src in (me - k, me + k):

                @pl.when((src >= 0) & (src < n))
                def _(src=src):
                    outs.arrive_shard(src, (0, 1))
                    project(src)

            return 0

        lax.fori_loop(1, n, out_step, 0)
    else:
        outs.arrive((0, 1))
        project(0)

    summed = rs_send[mine, :].astype(jnp.float32)
    for d in range(1, n_tp):
        for piece in range(pieces):
            rs_copy(d, piece).wait_recv()
        summed = summed + rs_buf[d - 1].astype(jnp.float32)
    out_ref[...] = summed.astype(jnp.bfloat16)

    for d in range(1, n_tp):
        tok_copy(d).wait_send()
        for piece in range(pieces):
            rs_copy(d, piece).wait_send()
    weights.finish()
    outs.finish()

    @pl.when(has_up)
    def _():
        def step(src, _):
            kv_copy(src).wait_send()
            sum_copy(src).wait_send()
            return 0

        lax.fori_loop(0, me + 1, step, 0)


def local(
    n,
    n_tp,
    n_grp,
    tokens,
    norm_gain,
    ret_query_weight,
    ret_key_weight,
    ret_value_weight,
    fox_query_weight,
    fox_key_weight,
    fox_value_weight,
    ret_decay,
    ret_state,
    head_norm_gain,
    fox_gates,
    ret_out_weight,
    fox_out_weight,
):
    rows, feats = tokens.shape
    hr, dk, vd = ret_state.shape
    fh = fox_gates.shape[1]
    fd = fox_query_weight.shape[1] // fh
    shard = ret_query_weight.shape[0]
    width = 2 * hr * dk + hr * vd + 3 * fh * fd
    depth, out_cols = ret_out_weight.shape
    columns = out_cols * n
    direct = out_cols % 128 == 0
    if not direct:
        ret_out_weight, fox_out_weight = ret_out_weight.T, fox_out_weight.T
    dma = pltpu.SemaphoreType.DMA

    def gather_sems(arrays):
        side = max(n_grp - 1, 1) * n * arrays
        return [
            dma((n * arrays,)),
            dma((n * arrays,)),
            dma((n * arrays,)),
            dma((side,)),
            dma((side,)),
            dma((arrays,)),
        ]

    vmem = pl.BlockSpec(memory_space=pltpu.VMEM)
    smem = pl.BlockSpec(memory_space=pltpu.SMEM)
    hbm = pl.BlockSpec(memory_space=pl.ANY)
    size = (n, n_tp, n_grp, hr, dk, vd, fh, fd, direct)
    block = rows // n_tp
    peers = max(n_tp - 1, 1)
    pieces = n if direct else 1
    return pl.pallas_call(
        functools.partial(kernel, size),
        out_shape=jax.ShapeDtypeStruct((block, columns), jnp.bfloat16),
        in_specs=[hbm, vmem, vmem, vmem, hbm, hbm, hbm, hbm, smem, vmem, vmem, vmem, hbm, hbm],
        out_specs=vmem,
        scratch_shapes=[
            pltpu.VMEM((n_tp, rows, feats), jnp.bfloat16),
            pltpu.VMEM((shard, 2 * hr * dk), jnp.bfloat16),
            pltpu.VMEM((n * shard, width), jnp.bfloat16),
            pltpu.VMEM((2 * depth, columns) if direct else (columns, 2 * depth), jnp.bfloat16),
            pltpu.VMEM((rows, n_tp * feats), jnp.bfloat16),
            pltpu.VMEM((rows, width - 2 * fh * fd), jnp.bfloat16),
            pltpu.VMEM((n, rows, 2 * fh * fd), jnp.bfloat16),
            pltpu.VMEM((n, hr, dk, vd), jnp.float32),
            pltpu.VMEM((rows, 2 * depth), jnp.bfloat16),
            pltpu.VMEM((rows, columns), jnp.bfloat16),
            pltpu.VMEM((peers, block, columns), jnp.bfloat16),
            pltpu.VMEM((fh, rows, 1), jnp.float32),
            pltpu.VMEM((fh, rows, 1), jnp.float32),
            pltpu.VMEM((fh, rows, fd), jnp.float32),
            dma((peers,)),
            dma((peers,)),
            dma,
            dma((n,)),
            dma((n,)),
            dma((n,)),
            dma((n,)),
            dma((peers * pieces,)),
            dma((peers * pieces,)),
        ]
        + gather_sems(5)
        + gather_sems(2),
        compiler_params=pltpu.CompilerParams(
            collective_id=0, has_side_effects=True, vmem_limit_bytes=56 * 1024 * 1024
        ),
        name="layer",
    )(
        tokens,
        norm_gain[None, :],
        ret_query_weight.T,
        ret_key_weight.T,
        ret_value_weight,
        fox_query_weight,
        fox_key_weight,
        fox_value_weight,
        ret_decay,
        ret_state,
        head_norm_gain[None, :],
        fox_gates.T,
        ret_out_weight,
        fox_out_weight,
    )


def solution(mesh):
    placed = (
        P(("grp", "sp"), "tp"),
        P(),
        P("sp", "tp"),
        P("sp", "tp"),
        P("sp", "tp"),
        P("sp", "tp"),
        P("sp", "tp"),
        P("sp", "tp"),
        P("tp"),
        P(("grp", "tp"), None, None),
        P("tp"),
        P("grp", "tp"),
        P("tp", "sp"),
        P("tp", "sp"),
    )
    body = functools.partial(local, mesh.shape["sp"], mesh.shape["tp"], mesh.shape["grp"])
    return jax.shard_map(
        body, mesh=mesh, in_specs=placed, out_specs=P(("grp", "sp", "tp"), None), check_vma=False
    )
```

```python
import functools

import jax
import jax.numpy as jnp
from jax import lax
from jax.experimental import pallas as pl
from jax.experimental.pallas import tpu as pltpu
from jax.sharding import PartitionSpec as P

epsilon = 1e-06
highest = lax.Precision.HIGHEST
NT = (((1,), (1,)), ((), ()))
TN = (((0,), (0,)), ((), ()))


def rdma(src, dst, send_sem, recv_sem, **target):
    return pltpu.make_async_remote_copy(
        src_ref=src,
        dst_ref=dst,
        send_sem=send_sem,
        recv_sem=recv_sem,
        device_id=target,
        device_id_type=pl.DeviceIdType.MESH,
    )


class LineGather:
    def __init__(self, owns, place, sems, n, n_grp, me, g):
        self.owns, self.place, self.n, self.n_grp, self.me, self.g = owns, place, n, n_grp, me, g
        self.up, self.down, self.zr, self.ys, self.yr, self.loc = sems
        self.arrays = len(owns)
        self.rows = owns[0].shape[0]
        self.step = self.rows // n_grp

    def piece(self, part, src, c):
        return self.place(src, c, part * self.step, self.step)

    def own_piece(self, c):
        return self.owns[c].at[pl.ds(pl.multiple_of(self.g * self.step, self.step), self.step)]

    def hop(self, sems, to, src, c, first=False):
        here = self.own_piece(c) if first else self.piece(self.g, src, c)
        at = src * self.arrays + c
        return rdma(here, self.piece(self.g, src, c), sems.at[at], self.zr.at[at], sp=to)

    def side(self, d, src, c):
        at = ((d - 1) * self.n + src) * self.arrays + c
        here = self.piece(self.g, src, c)
        return rdma(here, here, self.ys.at[at], self.yr.at[at], grp=lax.rem(self.g + d, self.n_grp))

    def side_in(self, d, src, c):
        at = ((d - 1) * self.n + src) * self.arrays + c
        part = lax.rem(self.g + self.n_grp - d, self.n_grp)
        here = self.piece(part, src, c)
        return rdma(here, here, self.ys.at[at], self.yr.at[at], grp=part)

    def local(self, c):
        return pltpu.make_async_copy(self.owns[c], self.place(self.me, c, 0, self.rows), self.loc.at[c])

    def start(self):
        me, n = self.me, self.n
        for c in range(self.arrays):

            @pl.when(me + 1 < n)
            def _():
                self.hop(self.up, me + 1, me, c, True).start()

            @pl.when(me >= 1)
            def _():
                self.hop(self.down, me - 1, me, c, True).start()

        for c in range(self.arrays):
            self.local(c).start()

    def relay(self, k):
        me, n = self.me, self.n
        for c in range(self.arrays):
            for src, sems, to in ((me - k, self.up, me + 1), (me + k, self.down, me - 1)):

                @pl.when((src >= 0) & (src < n))
                def _(src=src, sems=sems, to=to):
                    self.hop(sems, me, src, c).wait_recv()

                    @pl.when((to >= 0) & (to < n))
                    def _():
                        self.hop(sems, to, src, c).start()

                    for d in range(1, self.n_grp):
                        self.side(d, src, c).start()

    def arrive_shard(self, src, arrays):
        for c in arrays:
            for d in range(1, self.n_grp):
                self.side_in(d, src, c).wait_recv()

    def arrive(self, arrays):
        for c in arrays:
            self.local(c).wait()

        def step(k, _):
            self.arrive_shard(lax.rem(self.me + k, self.n), arrays)
            return 0

        lax.fori_loop(1, self.n, step, 0)

    def finish(self):
        me, n = self.me, self.n

        def step(src, _):
            for c in range(self.arrays):

                @pl.when((src <= me) & (me + 1 < n))
                def _():
                    self.hop(self.up, me, src, c).wait_send()

                @pl.when((src >= me) & (me >= 1))
                def _():
                    self.hop(self.down, me, src, c).wait_send()

                @pl.when(src != me)
                def _():
                    for d in range(1, self.n_grp):
                        self.side(d, src, c).wait_send()

            return 0

        lax.fori_loop(0, n, step, 0)


def kernel(
    size,
    tok_ref,
    gain_ref,
    wq_ref,
    wk_ref,
    wrv_ref,
    wfq_ref,
    wfk_ref,
    wfv_ref,
    decay_ref,
    state_ref,
    hgain_ref,
    gates_ref,
    ret_out_ref,
    fox_out_ref,
    out_ref,
    tok_buf,
    qk_own,
    w_buf,
    wout_buf,
    norm_buf,
    proj_buf,
    kv_buf,
    sum_buf,
    mix_buf,
    rs_send,
    pair_buf,
    pair_sum,
    rs_buf,
    top_buf,
    total_buf,
    weighted_buf,
    tok_s,
    tok_r,
    tok_loc,
    kv_s,
    kv_r,
    sum_s,
    sum_r,
    pair_s,
    pair_r,
    rs_s,
    rs_r,
    *gather_sems,
):
    n, n_tp, n_grp, hr, dk, vd, fh, fd, direct = size
    me, t, g = lax.axis_index("sp"), lax.axis_index("tp"), lax.axis_index("grp")
    rows, feats = tok_ref.shape
    owns = [wfk_ref, wfv_ref, wfq_ref, wrv_ref, qk_own]
    early = 2
    starts = [0]
    for own in owns:
        starts.append(starts[-1] + own.shape[1])
    shard = qk_own.shape[0]

    def weight_place(src, c, first, count):
        start = pl.multiple_of(src * shard + first, count)
        return w_buf.at[pl.ds(start, count), starts[c] : starts[c + 1]]

    depth = mix_buf.shape[1] // 2
    out_cols = ret_out_ref.shape[1] if direct else ret_out_ref.shape[0]

    def out_place(src, c, first, count):
        if direct:
            start = pl.multiple_of(c * depth + first, count)
            return wout_buf.at[pl.ds(start, count), pl.ds(pl.multiple_of(src * out_cols, out_cols), out_cols)]
        start = pl.multiple_of(src * out_cols + first, count)
        return wout_buf.at[pl.ds(start, count), c * depth : (c + 1) * depth]

    def late_place(src, c, first, count):
        return weight_place(src, c + early, first, count)

    firsts = LineGather(owns[:early], weight_place, gather_sems[:6], n, n_grp, me, g)
    lasts = LineGather(owns[early:], late_place, gather_sems[6:12], n, n_grp, me, g)
    outs = LineGather([ret_out_ref, fox_out_ref], out_place, gather_sems[12:], n, n_grp, me, g)

    barrier = pltpu.get_barrier_semaphore()

    def greet(**target):
        pl.semaphore_signal(barrier, inc=1, device_id=target, device_id_type=pl.DeviceIdType.MESH)

    has_up, has_down = me + 1 < n, me >= 1
    for d in range(1, n_tp):
        greet(tp=lax.rem(t + d, n_tp))
    for d in range(1, n_grp):
        greet(grp=lax.rem(g + d, n_grp))

    @pl.when(has_up)
    def _():
        greet(sp=me + 1)

    @pl.when(has_down)
    def _():
        greet(sp=me - 1)

    turned = jnp.concatenate((wq_ref[...], wk_ref[...]), axis=0).astype(jnp.float32)
    qk_own[...] = turned.T.astype(jnp.bfloat16)

    count = n_tp - 1 + n_grp - 1 + has_up.astype(jnp.int32) + has_down.astype(jnp.int32)
    pl.semaphore_wait(barrier, count)

    def tok_copy(d):
        return rdma(tok_ref, tok_buf.at[t], tok_s.at[d - 1], tok_r.at[d - 1], tp=lax.rem(t + d, n_tp))

    def tok_in(d):
        src = lax.rem(t + n_tp - d, n_tp)
        return rdma(tok_ref, tok_buf.at[src], tok_s.at[d - 1], tok_r.at[d - 1], tp=src)

    firsts.start()
    tok_local = pltpu.make_async_copy(tok_ref, tok_buf.at[t], tok_loc)
    for d in range(1, n_tp):
        tok_copy(d).start()
    tok_local.start()

    def first_step(k, _):
        firsts.relay(k)

        @pl.when(k == 1)
        def _():
            lasts.start()

        return 0

    lax.fori_loop(1, n, first_step, 0)

    tok_local.wait()
    for d in range(1, n_tp):
        tok_in(d).wait_recv()
    squares = jnp.zeros((rows, 1), jnp.float32)
    for i in range(n_tp):
        part = tok_buf[i].astype(jnp.float32)
        squares = squares + jnp.sum(part * part, axis=-1, keepdims=True)
    scale = lax.rsqrt(squares * (1.0 / (n_tp * feats)) + epsilon)
    for i in range(n_tp):
        part = tok_buf[i].astype(jnp.float32)
        cols = slice(i * feats, (i + 1) * feats)
        norm_buf[:, cols] = (part * scale * gain_ref[:, cols]).astype(jnp.bfloat16)

    def kv_copy(src):
        return rdma(kv_buf.at[src], kv_buf.at[src], kv_s.at[src], kv_r.at[src], sp=jnp.minimum(me + 1, n - 1))

    def sum_copy(src):
        return rdma(sum_buf.at[src], sum_buf.at[src], sum_s.at[src], sum_r.at[src], sp=jnp.minimum(me + 1, n - 1))

    firsts.arrive((0, 1))
    kv_buf[me] = jnp.dot(
        norm_buf[...], w_buf[:, : starts[2]], preferred_element_type=jnp.float32
    ).astype(jnp.bfloat16)

    def kv_forward(k):
        src = me - k

        @pl.when(src >= 0)
        def _():
            kv_copy(src).wait_recv()

            @pl.when(has_up)
            def _():
                kv_copy(src).start()

    @pl.when(has_up)
    def _():
        kv_copy(me).start()

    def last_step(k, _):
        lasts.relay(k)
        kv_forward(k)
        return 0

    lax.fori_loop(1, n, last_step, 0)
    outs.start()
    lasts.arrive((0, 1, 2))
    proj_buf[...] = jnp.dot(
        norm_buf[...], w_buf[:, starts[2] :], preferred_element_type=jnp.float32
    ).astype(jnp.bfloat16)
    rv_at, rq_at = starts[3] - starts[2], starts[4] - starts[2]

    key_scale = dk ** (-0.5)
    position = lax.broadcasted_iota(jnp.int32, (rows, 1), 0).astype(jnp.float32)
    rq, rk, rv = [], [], []
    for h in range(hr):
        rq.append(proj_buf[:, rq_at + h * dk : rq_at + (h + 1) * dk])
        rk.append(proj_buf[:, rq_at + (hr + h) * dk : rq_at + (hr + h + 1) * dk])
        rv.append(proj_buf[:, rv_at + h * vd : rv_at + (h + 1) * vd])
        keys = rk[h].astype(jnp.float32) * key_scale
        trailing = jnp.exp((rows - 1.0 - position) * decay_ref[h])
        sum_buf[me, h] = lax.dot_general(
            keys * trailing, rv[h].astype(jnp.float32), TN, precision=highest, preferred_element_type=jnp.float32
        )

    @pl.when(has_up)
    def _():
        sum_copy(me).start()

    row_id = lax.broadcasted_iota(jnp.int32, (rows, rows), 0)
    col_id = lax.broadcasted_iota(jnp.int32, (rows, rows), 1)
    causal = col_id <= row_id
    own_cols = pl.ds(pl.multiple_of(me * rows, rows), rows)
    own_gates = [
        jnp.sum(jnp.where(row_id == col_id, gates_ref[h : h + 1, own_cols], 0.0), axis=1, keepdims=True)
        for h in range(fh)
    ]

    def attend(src, diagonal):
        key_cols = pl.ds(pl.multiple_of(src * rows, rows), rows)
        for h in range(fh):
            query = proj_buf[:, h * fd : (h + 1) * fd]
            k = kv_buf[src, :, h * fd : (h + 1) * fd]
            v = kv_buf[src, :, (fh + h) * fd : (fh + h + 1) * fd]
            logits = lax.dot_general(query, k, NT, preferred_element_type=jnp.float32) * fd ** (-0.5)
            logits = logits + own_gates[h] - gates_ref[h : h + 1, key_cols]
            if diagonal:
                logits = jnp.where(causal, logits, -jnp.inf)
            top_new = jnp.max(logits, axis=-1, keepdims=True)
            if not diagonal:
                top = top_buf[h]
                top_new = jnp.maximum(top, top_new)
            p = jnp.exp(logits - top_new)
            total = jnp.sum(p, axis=-1, keepdims=True)
            weighted = jnp.dot(p.astype(jnp.bfloat16), v, preferred_element_type=jnp.float32)
            if not diagonal:
                rescale = jnp.exp(top - top_new)
                total = total_buf[h] * rescale + total
                weighted = weighted_buf[h] * rescale + weighted
            top_buf[h] = top_new
            total_buf[h] = total
            weighted_buf[h] = weighted

    def forward(k):
        src = me - k

        @pl.when(src >= 0)
        def _():
            sum_copy(src).wait_recv()

            @pl.when(has_up)
            def _():
                sum_copy(src).start()

    if n > 1:
        outs.relay(1)
    attend(me, True)

    offset = (me * rows).astype(jnp.float32)
    lone = jnp.zeros((dk, vd), jnp.float32)

    def step(k, entering):
        src = me - k
        forward(k)

        @pl.when(k + 1 < n)
        def _():
            outs.relay(k + 1)

        @pl.when(src >= 0)
        def _():
            attend(src, False)

        gap = ((k - 1) * rows).astype(jnp.float32)
        there = jnp.maximum(src, 0)
        return tuple(
            entering[h]
            + jnp.where(src >= 0, jnp.exp(lone + gap * decay_ref[h]) * sum_buf[there, h], 0.0)
            for h in range(hr)
        )

    entering = tuple(jnp.exp(lone + offset * decay_ref[h]) * state_ref[h] for h in range(hr))
    entering = lax.fori_loop(1, n, step, entering)

    distance = jnp.maximum(row_id - col_id, 0).astype(jnp.float32)
    for h in range(hr):
        scores = lax.dot_general(rq[h], rk[h], NT, preferred_element_type=jnp.float32) * key_scale
        scores = jnp.where(causal, scores * jnp.exp(distance * decay_ref[h]), 0.0)
        inner = jnp.dot(scores, rv[h].astype(jnp.float32), precision=highest, preferred_element_type=jnp.float32)
        leading = jnp.exp((position + 1.0) * decay_ref[h])
        carried = jnp.dot(
            rq[h].astype(jnp.float32), entering[h], precision=highest, preferred_element_type=jnp.float32
        )
        raw = inner + carried * leading
        center = raw - jnp.mean(raw, axis=-1, keepdims=True)
        variance = jnp.mean(center * center, axis=-1, keepdims=True)
        cols = slice(h * vd, (h + 1) * vd)
        mix_buf[:, cols] = (center * lax.rsqrt(variance + epsilon) * hgain_ref[:, cols]).astype(jnp.bfloat16)
    for h in range(fh):
        cols = slice(hr * vd + h * fd, hr * vd + (h + 1) * fd)
        mix_buf[:, cols] = (weighted_buf[h] / total_buf[h]).astype(jnp.bfloat16)

    block = rows // n_tp
    columns = pair_buf.shape[1]
    wide = out_cols if direct else columns
    pieces = columns // wide
    half = n_tp // 2
    parity, pair = lax.rem(t, 2), lax.div(t, 2)

    def piece_cols(piece):
        return pl.ds(pl.multiple_of(piece * wide, wide), wide)

    def slot(at):
        return pl.ds(pl.multiple_of(at * block, block), block)

    def pair_copy(piece):
        cols = piece_cols(piece)
        return rdma(
            rs_send.at[1 - parity, :, cols],
            pair_buf.at[:, cols],
            pair_s.at[piece],
            pair_r.at[piece],
            tp=t + 1 - 2 * parity,
        )

    def rs_copy(d, piece):
        to = lax.rem(pair + d, half)
        cols = piece_cols(piece)
        at = (d - 1) * pieces + piece
        return rdma(
            pair_sum.at[slot(to), cols], rs_buf.at[d - 1, :, cols], rs_s.at[at], rs_r.at[at], tp=2 * to + parity
        )

    def project(piece):
        cols = piece_cols(piece)
        if direct:
            value = jnp.dot(mix_buf[...], wout_buf[:, cols], preferred_element_type=jnp.float32)
        else:
            value = lax.dot_general(mix_buf[...], wout_buf[...], NT, preferred_element_type=jnp.float32)
        value = value.astype(jnp.bfloat16)
        for b in range(n_tp):
            at = slice(b // 2 * block, (b // 2 + 1) * block)
            rs_send[b % 2, at, cols] = value[b * block : (b + 1) * block]
        pair_copy(piece).start()

    def reduce(piece):
        cols = piece_cols(piece)
        pair_copy(piece).wait_recv()
        both = rs_send[parity, :, cols].astype(jnp.float32) + pair_buf[:, cols].astype(jnp.float32)
        pair_sum[:, cols] = both.astype(jnp.bfloat16)
        for d in range(1, half):
            rs_copy(d, piece).start()

    def order(i):
        falling = jnp.where(i <= me, me - i, i)
        rising = jnp.where(i <= n - 1 - me, me + i, n - 1 - i)
        return jnp.where(2 * me >= n, falling, rising)

    if direct:
        for c in range(2):
            outs.local(c).wait()
        project(me)

        def out_step(i, _):
            outs.arrive_shard(order(i), (0, 1))
            project(order(i))
            reduce(order(i - 1))
            return 0

        lax.fori_loop(1, n, out_step, 0)
        reduce(order(jnp.int32(n - 1)))
    else:
        outs.arrive((0, 1))
        project(0)
        reduce(0)

    own = slot(pair)
    summed = rs_send[parity, own, :].astype(jnp.float32) + pair_buf[own, :].astype(jnp.float32)
    for d in range(1, half):
        for piece in range(pieces):
            rs_copy(d, piece).wait_recv()
        summed = summed + rs_buf[d - 1].astype(jnp.float32)
    out_ref[...] = summed.astype(jnp.bfloat16)

    for d in range(1, n_tp):
        tok_copy(d).wait_send()
    for piece in range(pieces):
        pair_copy(piece).wait_send()
        for d in range(1, half):
            rs_copy(d, piece).wait_send()
    firsts.finish()
    lasts.finish()
    outs.finish()

    @pl.when(has_up)
    def _():
        def step(src, _):
            kv_copy(src).wait_send()
            sum_copy(src).wait_send()
            return 0

        lax.fori_loop(0, me + 1, step, 0)


def local(
    n,
    n_tp,
    n_grp,
    tokens,
    norm_gain,
    ret_query_weight,
    ret_key_weight,
    ret_value_weight,
    fox_query_weight,
    fox_key_weight,
    fox_value_weight,
    ret_decay,
    ret_state,
    head_norm_gain,
    fox_gates,
    ret_out_weight,
    fox_out_weight,
):
    rows, feats = tokens.shape
    hr, dk, vd = ret_state.shape
    fh = fox_gates.shape[1]
    fd = fox_query_weight.shape[1] // fh
    shard = ret_query_weight.shape[0]
    width = 2 * hr * dk + hr * vd + 3 * fh * fd
    depth, out_cols = ret_out_weight.shape
    columns = out_cols * n
    direct = out_cols % 128 == 0
    if not direct:
        ret_out_weight, fox_out_weight = ret_out_weight.T, fox_out_weight.T
    dma = pltpu.SemaphoreType.DMA

    def gather_sems(arrays):
        side = max(n_grp - 1, 1) * n * arrays
        return [
            dma((n * arrays,)),
            dma((n * arrays,)),
            dma((n * arrays,)),
            dma((side,)),
            dma((side,)),
            dma((arrays,)),
        ]

    vmem = pl.BlockSpec(memory_space=pltpu.VMEM)
    smem = pl.BlockSpec(memory_space=pltpu.SMEM)
    hbm = pl.BlockSpec(memory_space=pl.ANY)
    size = (n, n_tp, n_grp, hr, dk, vd, fh, fd, direct)
    block = rows // n_tp
    peers = max(n_tp - 1, 1)
    far = max(n_tp // 2 - 1, 1)
    pieces = n if direct else 1
    return pl.pallas_call(
        functools.partial(kernel, size),
        out_shape=jax.ShapeDtypeStruct((block, columns), jnp.bfloat16),
        in_specs=[hbm, vmem, vmem, vmem, hbm, hbm, hbm, hbm, smem, vmem, vmem, vmem, hbm, hbm],
        out_specs=vmem,
        scratch_shapes=[
            pltpu.VMEM((n_tp, rows, feats), jnp.bfloat16),
            pltpu.VMEM((shard, 2 * hr * dk), jnp.bfloat16),
            pltpu.VMEM((n * shard, width), jnp.bfloat16),
            pltpu.VMEM((2 * depth, columns) if direct else (columns, 2 * depth), jnp.bfloat16),
            pltpu.VMEM((rows, n_tp * feats), jnp.bfloat16),
            pltpu.VMEM((rows, width - 2 * fh * fd), jnp.bfloat16),
            pltpu.VMEM((n, rows, 2 * fh * fd), jnp.bfloat16),
            pltpu.VMEM((n, hr, dk, vd), jnp.float32),
            pltpu.VMEM((rows, 2 * depth), jnp.bfloat16),
            pltpu.VMEM((2, rows // 2, columns), jnp.bfloat16),
            pltpu.VMEM((rows // 2, columns), jnp.bfloat16),
            pltpu.VMEM((rows // 2, columns), jnp.bfloat16),
            pltpu.VMEM((far, block, columns), jnp.bfloat16),
            pltpu.VMEM((fh, rows, 1), jnp.float32),
            pltpu.VMEM((fh, rows, 1), jnp.float32),
            pltpu.VMEM((fh, rows, fd), jnp.float32),
            dma((peers,)),
            dma((peers,)),
            dma,
            dma((n,)),
            dma((n,)),
            dma((n,)),
            dma((n,)),
            dma((pieces,)),
            dma((pieces,)),
            dma((far * pieces,)),
            dma((far * pieces,)),
        ]
        + gather_sems(2)
        + gather_sems(3)
        + gather_sems(2),
        compiler_params=pltpu.CompilerParams(
            collective_id=0, has_side_effects=True, vmem_limit_bytes=32 * 1024 * 1024
        ),
        name="layer",
    )(
        tokens,
        norm_gain[None, :],
        ret_query_weight.T,
        ret_key_weight.T,
        ret_value_weight,
        fox_query_weight,
        fox_key_weight,
        fox_value_weight,
        ret_decay,
        ret_state,
        head_norm_gain[None, :],
        fox_gates.T,
        ret_out_weight,
        fox_out_weight,
    )


def solution(mesh):
    placed = (
        P(("grp", "sp"), "tp"),
        P(),
        P("sp", "tp"),
        P("sp", "tp"),
        P("sp", "tp"),
        P("sp", "tp"),
        P("sp", "tp"),
        P("sp", "tp"),
        P("tp"),
        P(("grp", "tp"), None, None),
        P("tp"),
        P("grp", "tp"),
        P("tp", "sp"),
        P("tp", "sp"),
    )
    body = functools.partial(local, mesh.shape["sp"], mesh.shape["tp"], mesh.shape["grp"])
    return jax.shard_map(
        body, mesh=mesh, in_specs=placed, out_specs=P(("grp", "sp", "tp"), None), check_vma=False
    )
```

```python
import functools

import jax
import jax.numpy as jnp
from jax import lax
from jax.experimental import pallas as pl
from jax.experimental.pallas import tpu as pltpu
from jax.sharding import PartitionSpec as P

epsilon = 1e-06
highest = lax.Precision.HIGHEST
NT = (((1,), (1,)), ((), ()))
TN = (((0,), (0,)), ((), ()))


def rdma(src, dst, send_sem, recv_sem, **target):
    return pltpu.make_async_remote_copy(
        src_ref=src,
        dst_ref=dst,
        send_sem=send_sem,
        recv_sem=recv_sem,
        device_id=target,
        device_id_type=pl.DeviceIdType.MESH,
    )


class LineGather:
    def __init__(self, owns, place, sems, n, n_grp, me, g):
        self.owns, self.place, self.n, self.n_grp, self.me, self.g = owns, place, n, n_grp, me, g
        self.up, self.down, self.zr, self.ys, self.yr, self.loc = sems
        self.arrays = len(owns)
        self.rows = owns[0].shape[0]
        self.step = self.rows // n_grp

    def piece(self, part, src, c):
        return self.place(src, c, part * self.step, self.step)

    def own_piece(self, c):
        return self.owns[c].at[pl.ds(pl.multiple_of(self.g * self.step, self.step), self.step)]

    def hop(self, sems, to, src, c, first=False):
        here = self.own_piece(c) if first else self.piece(self.g, src, c)
        at = src * self.arrays + c
        return rdma(here, self.piece(self.g, src, c), sems.at[at], self.zr.at[at], sp=to)

    def side(self, d, src, c):
        at = ((d - 1) * self.n + src) * self.arrays + c
        here = self.piece(self.g, src, c)
        return rdma(here, here, self.ys.at[at], self.yr.at[at], grp=lax.rem(self.g + d, self.n_grp))

    def side_in(self, d, src, c):
        at = ((d - 1) * self.n + src) * self.arrays + c
        part = lax.rem(self.g + self.n_grp - d, self.n_grp)
        here = self.piece(part, src, c)
        return rdma(here, here, self.ys.at[at], self.yr.at[at], grp=part)

    def local(self, c):
        return pltpu.make_async_copy(self.owns[c], self.place(self.me, c, 0, self.rows), self.loc.at[c])

    def start(self):
        me, n = self.me, self.n
        for c in range(self.arrays):

            @pl.when(me + 1 < n)
            def _():
                self.hop(self.up, me + 1, me, c, True).start()

            @pl.when(me >= 1)
            def _():
                self.hop(self.down, me - 1, me, c, True).start()

        for c in range(self.arrays):
            self.local(c).start()

    def relay(self, k):
        me, n = self.me, self.n
        for c in range(self.arrays):
            for src, sems, to in ((me - k, self.up, me + 1), (me + k, self.down, me - 1)):

                @pl.when((src >= 0) & (src < n))
                def _(src=src, sems=sems, to=to):
                    self.hop(sems, me, src, c).wait_recv()

                    @pl.when((to >= 0) & (to < n))
                    def _():
                        self.hop(sems, to, src, c).start()

                    for d in range(1, self.n_grp):
                        self.side(d, src, c).start()

    def arrive_shard(self, src, arrays):
        for c in arrays:
            for d in range(1, self.n_grp):
                self.side_in(d, src, c).wait_recv()

    def arrive(self, arrays):
        for c in arrays:
            self.local(c).wait()

        def step(k, _):
            self.arrive_shard(lax.rem(self.me + k, self.n), arrays)
            return 0

        lax.fori_loop(1, self.n, step, 0)

    def finish(self):
        me, n = self.me, self.n

        def step(src, _):
            for c in range(self.arrays):

                @pl.when((src <= me) & (me + 1 < n))
                def _():
                    self.hop(self.up, me, src, c).wait_send()

                @pl.when((src >= me) & (me >= 1))
                def _():
                    self.hop(self.down, me, src, c).wait_send()

                @pl.when(src != me)
                def _():
                    for d in range(1, self.n_grp):
                        self.side(d, src, c).wait_send()

            return 0

        lax.fori_loop(0, n, step, 0)


def kernel(
    size,
    tok_ref,
    gain_ref,
    wq_ref,
    wk_ref,
    wrv_ref,
    wfq_ref,
    wfk_ref,
    wfv_ref,
    decay_ref,
    state_ref,
    hgain_ref,
    gates_ref,
    ret_out_ref,
    fox_out_ref,
    out_ref,
    tok_buf,
    qk_own,
    w_buf,
    wout_buf,
    norm_buf,
    proj_buf,
    kv_buf,
    sum_buf,
    mix_buf,
    rs_send,
    pair_buf,
    pair_sum,
    rs_buf,
    top_buf,
    total_buf,
    weighted_buf,
    tok_s,
    tok_r,
    tok_loc,
    kv_s,
    kv_r,
    sum_s,
    sum_r,
    pair_s,
    pair_r,
    rs_s,
    rs_r,
    *gather_sems,
):
    n, n_tp, n_grp, hr, dk, vd, fh, fd, direct = size
    me, t, g = lax.axis_index("sp"), lax.axis_index("tp"), lax.axis_index("grp")
    rows, feats = tok_ref.shape
    owns = [wfk_ref, wfv_ref, wfq_ref, wrv_ref, qk_own]
    early = 2
    starts = [0]
    for own in owns:
        starts.append(starts[-1] + own.shape[1])
    shard = qk_own.shape[0]

    def weight_place(src, c, first, count):
        start = pl.multiple_of(src * shard + first, count)
        return w_buf.at[pl.ds(start, count), starts[c] : starts[c + 1]]

    depth = mix_buf.shape[1] // 2
    out_cols = ret_out_ref.shape[1] if direct else ret_out_ref.shape[0]

    def out_place(src, c, first, count):
        if direct:
            start = pl.multiple_of(c * depth + first, count)
            return wout_buf.at[pl.ds(start, count), pl.ds(pl.multiple_of(src * out_cols, out_cols), out_cols)]
        start = pl.multiple_of(src * out_cols + first, count)
        return wout_buf.at[pl.ds(start, count), c * depth : (c + 1) * depth]

    def late_place(src, c, first, count):
        return weight_place(src, c + early, first, count)

    firsts = LineGather(owns[:early], weight_place, gather_sems[:6], n, n_grp, me, g)
    lasts = LineGather(owns[early:], late_place, gather_sems[6:12], n, n_grp, me, g)
    outs = LineGather([ret_out_ref, fox_out_ref], out_place, gather_sems[12:], n, n_grp, me, g)

    barrier = pltpu.get_barrier_semaphore()

    def greet(**target):
        pl.semaphore_signal(barrier, inc=1, device_id=target, device_id_type=pl.DeviceIdType.MESH)

    has_up, has_down = me + 1 < n, me >= 1
    for d in range(1, n_tp):
        greet(tp=lax.rem(t + d, n_tp))
    for d in range(1, n_grp):
        greet(grp=lax.rem(g + d, n_grp))

    @pl.when(has_up)
    def _():
        greet(sp=me + 1)

    @pl.when(has_down)
    def _():
        greet(sp=me - 1)

    turned = jnp.concatenate((wq_ref[...], wk_ref[...]), axis=0).astype(jnp.float32)
    qk_own[...] = turned.T.astype(jnp.bfloat16)

    count = n_tp - 1 + n_grp - 1 + has_up.astype(jnp.int32) + has_down.astype(jnp.int32)
    pl.semaphore_wait(barrier, count)

    def tok_copy(d):
        return rdma(tok_ref, tok_buf.at[t], tok_s.at[d - 1], tok_r.at[d - 1], tp=lax.rem(t + d, n_tp))

    def tok_in(d):
        src = lax.rem(t + n_tp - d, n_tp)
        return rdma(tok_ref, tok_buf.at[src], tok_s.at[d - 1], tok_r.at[d - 1], tp=src)

    firsts.start()
    lasts.start()
    tok_local = pltpu.make_async_copy(tok_ref, tok_buf.at[t], tok_loc)
    for d in range(1, n_tp):
        tok_copy(d).start()
    tok_local.start()

    def first_step(k, _):
        firsts.relay(k)

        lasts.relay(k)
        return 0

    lax.fori_loop(1, n, first_step, 0)
    outs.start()

    tok_local.wait()
    for d in range(1, n_tp):
        tok_in(d).wait_recv()
    squares = jnp.zeros((rows, 1), jnp.float32)
    for i in range(n_tp):
        part = tok_buf[i].astype(jnp.float32)
        squares = squares + jnp.sum(part * part, axis=-1, keepdims=True)
    scale = lax.rsqrt(squares * (1.0 / (n_tp * feats)) + epsilon)
    for i in range(n_tp):
        part = tok_buf[i].astype(jnp.float32)
        cols = slice(i * feats, (i + 1) * feats)
        norm_buf[:, cols] = (part * scale * gain_ref[:, cols]).astype(jnp.bfloat16)

    def kv_copy(src):
        return rdma(kv_buf.at[src], kv_buf.at[src], kv_s.at[src], kv_r.at[src], sp=jnp.minimum(me + 1, n - 1))

    def sum_copy(src):
        return rdma(sum_buf.at[src], sum_buf.at[src], sum_s.at[src], sum_r.at[src], sp=jnp.minimum(me + 1, n - 1))

    firsts.arrive((0, 1))
    kv_buf[me] = jnp.dot(
        norm_buf[...], w_buf[:, : starts[2]], preferred_element_type=jnp.float32
    ).astype(jnp.bfloat16)

    def kv_forward(k):
        src = me - k

        @pl.when(src >= 0)
        def _():
            kv_copy(src).wait_recv()

            @pl.when(has_up)
            def _():
                kv_copy(src).start()

    @pl.when(has_up)
    def _():
        kv_copy(me).start()

    outs.relay(1)
    lasts.arrive((0, 1, 2))
    proj_buf[...] = jnp.dot(
        norm_buf[...], w_buf[:, starts[2] :], preferred_element_type=jnp.float32
    ).astype(jnp.bfloat16)
    rv_at, rq_at = starts[3] - starts[2], starts[4] - starts[2]

    key_scale = dk ** (-0.5)
    position = lax.broadcasted_iota(jnp.int32, (rows, 1), 0).astype(jnp.float32)
    rq, rk, rv = [], [], []
    for h in range(hr):
        rq.append(proj_buf[:, rq_at + h * dk : rq_at + (h + 1) * dk])
        rk.append(proj_buf[:, rq_at + (hr + h) * dk : rq_at + (hr + h + 1) * dk])
        rv.append(proj_buf[:, rv_at + h * vd : rv_at + (h + 1) * vd])
        keys = rk[h].astype(jnp.float32) * key_scale
        trailing = jnp.exp((rows - 1.0 - position) * decay_ref[h])
        sum_buf[me, h] = lax.dot_general(
            keys * trailing, rv[h].astype(jnp.float32), TN, precision=highest, preferred_element_type=jnp.float32
        )

    @pl.when(has_up)
    def _():
        sum_copy(me).start()

    row_id = lax.broadcasted_iota(jnp.int32, (rows, rows), 0)
    col_id = lax.broadcasted_iota(jnp.int32, (rows, rows), 1)
    causal = col_id <= row_id
    own_cols = pl.ds(pl.multiple_of(me * rows, rows), rows)
    own_gates = [
        jnp.sum(jnp.where(row_id == col_id, gates_ref[h : h + 1, own_cols], 0.0), axis=1, keepdims=True)
        for h in range(fh)
    ]

    def attend(src, diagonal):
        key_cols = pl.ds(pl.multiple_of(src * rows, rows), rows)
        for h in range(fh):
            query = proj_buf[:, h * fd : (h + 1) * fd]
            k = kv_buf[src, :, h * fd : (h + 1) * fd]
            v = kv_buf[src, :, (fh + h) * fd : (fh + h + 1) * fd]
            logits = lax.dot_general(query, k, NT, preferred_element_type=jnp.float32) * fd ** (-0.5)
            logits = logits + own_gates[h] - gates_ref[h : h + 1, key_cols]
            if diagonal:
                logits = jnp.where(causal, logits, -jnp.inf)
            top_new = jnp.max(logits, axis=-1, keepdims=True)
            if not diagonal:
                top = top_buf[h]
                top_new = jnp.maximum(top, top_new)
            p = jnp.exp(logits - top_new)
            total = jnp.sum(p, axis=-1, keepdims=True)
            weighted = jnp.dot(p.astype(jnp.bfloat16), v, preferred_element_type=jnp.float32)
            if not diagonal:
                rescale = jnp.exp(top - top_new)
                total = total_buf[h] * rescale + total
                weighted = weighted_buf[h] * rescale + weighted
            top_buf[h] = top_new
            total_buf[h] = total
            weighted_buf[h] = weighted

    def forward(k):
        src = me - k

        @pl.when(src >= 0)
        def _():
            sum_copy(src).wait_recv()

            @pl.when(has_up)
            def _():
                sum_copy(src).start()

    attend(me, True)

    offset = (me * rows).astype(jnp.float32)
    lone = jnp.zeros((dk, vd), jnp.float32)

    def step(k, entering):
        src = me - k
        kv_forward(k)
        forward(k)

        @pl.when(k + 1 < n)
        def _():
            outs.relay(k + 1)


        @pl.when(src >= 0)
        def _():
            attend(src, False)

        gap = ((k - 1) * rows).astype(jnp.float32)
        there = jnp.maximum(src, 0)
        return tuple(
            entering[h]
            + jnp.where(src >= 0, jnp.exp(lone + gap * decay_ref[h]) * sum_buf[there, h], 0.0)
            for h in range(hr)
        )

    entering = tuple(jnp.exp(lone + offset * decay_ref[h]) * state_ref[h] for h in range(hr))
    entering = lax.fori_loop(1, n, step, entering)

    distance = jnp.maximum(row_id - col_id, 0).astype(jnp.float32)
    for h in range(hr):
        scores = lax.dot_general(rq[h], rk[h], NT, preferred_element_type=jnp.float32) * key_scale
        scores = jnp.where(causal, scores * jnp.exp(distance * decay_ref[h]), 0.0)
        inner = jnp.dot(scores, rv[h].astype(jnp.float32), precision=highest, preferred_element_type=jnp.float32)
        leading = jnp.exp((position + 1.0) * decay_ref[h])
        carried = jnp.dot(
            rq[h].astype(jnp.float32), entering[h], precision=highest, preferred_element_type=jnp.float32
        )
        raw = inner + carried * leading
        center = raw - jnp.mean(raw, axis=-1, keepdims=True)
        variance = jnp.mean(center * center, axis=-1, keepdims=True)
        cols = slice(h * vd, (h + 1) * vd)
        mix_buf[:, cols] = (center * lax.rsqrt(variance + epsilon) * hgain_ref[:, cols]).astype(jnp.bfloat16)
    for h in range(fh):
        cols = slice(hr * vd + h * fd, hr * vd + (h + 1) * fd)
        mix_buf[:, cols] = (weighted_buf[h] / total_buf[h]).astype(jnp.bfloat16)

    block = rows // n_tp
    columns = pair_buf.shape[1]
    wide = out_cols if direct else columns
    pieces = columns // wide
    half = n_tp // 2
    parity, pair = lax.rem(t, 2), lax.div(t, 2)

    def piece_cols(piece):
        return pl.ds(pl.multiple_of(piece * wide, wide), wide)

    def slot(at):
        return pl.ds(pl.multiple_of(at * block, block), block)

    def pair_copy(piece):
        cols = piece_cols(piece)
        return rdma(
            rs_send.at[1 - parity, :, cols],
            pair_buf.at[:, cols],
            pair_s.at[piece],
            pair_r.at[piece],
            tp=t + 1 - 2 * parity,
        )

    def rs_copy(d, piece):
        to = lax.rem(pair + d, half)
        cols = piece_cols(piece)
        at = (d - 1) * pieces + piece
        return rdma(
            pair_sum.at[slot(to), cols], rs_buf.at[d - 1, :, cols], rs_s.at[at], rs_r.at[at], tp=2 * to + parity
        )

    def project(piece):
        cols = piece_cols(piece)
        if direct:
            value = jnp.dot(mix_buf[...], wout_buf[:, cols], preferred_element_type=jnp.float32)
        else:
            value = lax.dot_general(mix_buf[...], wout_buf[...], NT, preferred_element_type=jnp.float32)
        value = value.astype(jnp.bfloat16)
        for b in range(n_tp):
            at = slice(b // 2 * block, (b // 2 + 1) * block)
            rs_send[b % 2, at, cols] = value[b * block : (b + 1) * block]
        pair_copy(piece).start()

    def reduce(piece):
        cols = piece_cols(piece)
        pair_copy(piece).wait_recv()
        both = rs_send[parity, :, cols].astype(jnp.float32) + pair_buf[:, cols].astype(jnp.float32)
        pair_sum[:, cols] = both.astype(jnp.bfloat16)
        for d in range(1, half):
            rs_copy(d, piece).start()

    def order(i):
        falling = jnp.where(i <= me, me - i, i)
        rising = jnp.where(i <= n - 1 - me, me + i, n - 1 - i)
        return jnp.where(2 * me >= n, falling, rising)

    if direct:
        for c in range(2):
            outs.local(c).wait()
        project(me)

        def out_step(i, _):
            outs.arrive_shard(order(i), (0, 1))
            project(order(i))
            reduce(order(i - 1))
            return 0

        lax.fori_loop(1, n, out_step, 0)
        reduce(order(jnp.int32(n - 1)))
    else:
        outs.arrive((0, 1))
        project(0)
        reduce(0)

    own = slot(pair)
    summed = rs_send[parity, own, :].astype(jnp.float32) + pair_buf[own, :].astype(jnp.float32)
    for d in range(1, half):
        for piece in range(pieces):
            rs_copy(d, piece).wait_recv()
        summed = summed + rs_buf[d - 1].astype(jnp.float32)
    out_ref[...] = summed.astype(jnp.bfloat16)

    for d in range(1, n_tp):
        tok_copy(d).wait_send()
    for piece in range(pieces):
        pair_copy(piece).wait_send()
        for d in range(1, half):
            rs_copy(d, piece).wait_send()
    firsts.finish()
    lasts.finish()
    outs.finish()

    @pl.when(has_up)
    def _():
        def step(src, _):
            kv_copy(src).wait_send()
            sum_copy(src).wait_send()
            return 0

        lax.fori_loop(0, me + 1, step, 0)


def local(
    n,
    n_tp,
    n_grp,
    tokens,
    norm_gain,
    ret_query_weight,
    ret_key_weight,
    ret_value_weight,
    fox_query_weight,
    fox_key_weight,
    fox_value_weight,
    ret_decay,
    ret_state,
    head_norm_gain,
    fox_gates,
    ret_out_weight,
    fox_out_weight,
):
    rows, feats = tokens.shape
    hr, dk, vd = ret_state.shape
    fh = fox_gates.shape[1]
    fd = fox_query_weight.shape[1] // fh
    shard = ret_query_weight.shape[0]
    width = 2 * hr * dk + hr * vd + 3 * fh * fd
    depth, out_cols = ret_out_weight.shape
    columns = out_cols * n
    direct = out_cols % 128 == 0
    if not direct:
        ret_out_weight, fox_out_weight = ret_out_weight.T, fox_out_weight.T
    dma = pltpu.SemaphoreType.DMA

    def gather_sems(arrays):
        side = max(n_grp - 1, 1) * n * arrays
        return [
            dma((n * arrays,)),
            dma((n * arrays,)),
            dma((n * arrays,)),
            dma((side,)),
            dma((side,)),
            dma((arrays,)),
        ]

    vmem = pl.BlockSpec(memory_space=pltpu.VMEM)
    smem = pl.BlockSpec(memory_space=pltpu.SMEM)
    hbm = pl.BlockSpec(memory_space=pl.ANY)
    size = (n, n_tp, n_grp, hr, dk, vd, fh, fd, direct)
    block = rows // n_tp
    peers = max(n_tp - 1, 1)
    far = max(n_tp // 2 - 1, 1)
    pieces = n if direct else 1
    return pl.pallas_call(
        functools.partial(kernel, size),
        out_shape=jax.ShapeDtypeStruct((block, columns), jnp.bfloat16),
        in_specs=[hbm, vmem, vmem, vmem, hbm, hbm, hbm, hbm, smem, vmem, vmem, vmem, hbm, hbm],
        out_specs=vmem,
        scratch_shapes=[
            pltpu.VMEM((n_tp, rows, feats), jnp.bfloat16),
            pltpu.VMEM((shard, 2 * hr * dk), jnp.bfloat16),
            pltpu.VMEM((n * shard, width), jnp.bfloat16),
            pltpu.VMEM((2 * depth, columns) if direct else (columns, 2 * depth), jnp.bfloat16),
            pltpu.VMEM((rows, n_tp * feats), jnp.bfloat16),
            pltpu.VMEM((rows, width - 2 * fh * fd), jnp.bfloat16),
            pltpu.VMEM((n, rows, 2 * fh * fd), jnp.bfloat16),
            pltpu.VMEM((n, hr, dk, vd), jnp.float32),
            pltpu.VMEM((rows, 2 * depth), jnp.bfloat16),
            pltpu.VMEM((2, rows // 2, columns), jnp.bfloat16),
            pltpu.VMEM((rows // 2, columns), jnp.bfloat16),
            pltpu.VMEM((rows // 2, columns), jnp.bfloat16),
            pltpu.VMEM((far, block, columns), jnp.bfloat16),
            pltpu.VMEM((fh, rows, 1), jnp.float32),
            pltpu.VMEM((fh, rows, 1), jnp.float32),
            pltpu.VMEM((fh, rows, fd), jnp.float32),
            dma((peers,)),
            dma((peers,)),
            dma,
            dma((n,)),
            dma((n,)),
            dma((n,)),
            dma((n,)),
            dma((pieces,)),
            dma((pieces,)),
            dma((far * pieces,)),
            dma((far * pieces,)),
        ]
        + gather_sems(2)
        + gather_sems(3)
        + gather_sems(2),
        compiler_params=pltpu.CompilerParams(
            collective_id=0, has_side_effects=True, vmem_limit_bytes=56 * 1024 * 1024
        ),
        name="layer",
    )(
        tokens,
        norm_gain[None, :],
        ret_query_weight.T,
        ret_key_weight.T,
        ret_value_weight,
        fox_query_weight,
        fox_key_weight,
        fox_value_weight,
        ret_decay,
        ret_state,
        head_norm_gain[None, :],
        fox_gates.T,
        ret_out_weight,
        fox_out_weight,
    )


def solution(mesh):
    placed = (
        P(("grp", "sp"), "tp"),
        P(),
        P("sp", "tp"),
        P("sp", "tp"),
        P("sp", "tp"),
        P("sp", "tp"),
        P("sp", "tp"),
        P("sp", "tp"),
        P("tp"),
        P(("grp", "tp"), None, None),
        P("tp"),
        P("grp", "tp"),
        P("tp", "sp"),
        P("tp", "sp"),
    )
    body = functools.partial(local, mesh.shape["sp"], mesh.shape["tp"], mesh.shape["grp"])
    return jax.shard_map(
        body, mesh=mesh, in_specs=placed, out_specs=P(("grp", "sp", "tp"), None), check_vma=False
    )
```
